32 devices in a mesh: sp: 4 (over y, x), tp: 8 (over z, core).
Axes of the slice: x: 2, y: 2, z: 4, core: 2. Of those that a mesh axis runs over, the one named last changes fastest.
Arguments:
- latent: bfloat16 [2048, 4096], P(('sp', 'tp')), may hold values from -6 to 6
- context: bfloat16 [512, 4096], P('sp'), may hold values from -6 to 6
- condition: float32 [4096], replicated, may hold values from -6 to 6
- context_condition: float32 [4096], replicated, may hold values from -6 to 6
- modulation: bfloat16 [3, 4096, 4096], P(None, 'sp', 'tp'), may hold values from -0.09375 to 0.09375
- query_weight: bfloat16 [4096, 4096], P(None, 'tp'), as said below
- key_weight: bfloat16 [4096, 4096], P(None, 'tp'), as said below
- value_weight: bfloat16 [4096, 4096], P(None, 'tp'), may hold values from -0.09375 to 0.09375
- lambdas: float32 [16], P('tp'), may hold values from 0.3 to 0.8
- context_lift: float32 [16], P('tp'), may hold values from 1.5 to 3
- head_gain: float32 [256], replicated, may hold values from 0.1 to 1.9
- output_weight: bfloat16 [4096, 4096], P('tp'), may hold values from -0.09375 to 0.09375
Outputs:
- result: bfloat16 [2048, 4096], P(('sp', 'tp'))
The draws below stay inside these ranges and needn't reach their ends.
Inputs may be any that keep to these rules, and one draw needn't show every extreme that they name: `query_weight`: entries lie within 200 / sqrt(4096) in magnitude. `key_weight`: entries lie within 6 / sqrt(4096) in magnitude.
All inputs are finite; a program needn't handle non-finite values.
Results may differ from the reference program's by a relative error of at most 0.025.
Values may be sent and summed in bfloat16 or wider, within the bound.
A program may use at most 64 MiB of HBM per device.

```python
import math
import jax
import jax.numpy as jnp
from jax import lax

D = 4096
HEADS = 16
HEAD_DIM = 256
GRID_W = 64
CTX = 512
SEQ = 2048


def common_keys(key):
    gaussian = jax.random.normal(jax.random.fold_in(key, 101), (D, HEADS * HEAD_DIM), jnp.float32)
    return jnp.clip(gaussian, -6.0, 6.0) * D ** (-0.5)


def draw_key_weight(key, part):
    return common_keys(key).astype(jnp.bfloat16)


def draw_query_weight(key, part):
    gaussian = jax.random.normal(jax.random.fold_in(key, 202), (D, HEADS * HEAD_DIM), jnp.float32)
    independent = jnp.clip(gaussian, -6.0, 6.0) * D ** (-0.5)
    return independent.astype(jnp.bfloat16)


def steps_of(rng, extent, shards, low, high):
    gain, own = 1.0, jax.random.fold_in(rng, 6)
    for dim, shards_of in shards:
        heights = jnp.exp(jax.random.uniform(jax.random.fold_in(own, dim), (shards_of,), jnp.float32, low / len(shards), high / len(shards)))
        gain = gain * jnp.repeat(heights, extent[dim] // shards_of).reshape([-1 if axis == dim else 1 for axis in range(len(extent))])
    return gain


def scatter_about(own_key, extent, scale, reach, cuts=(), kind=jnp.bfloat16):
    factor_of = steps_of(own_key, extent, cuts, -0.22, 0.18) if cuts else 1.0
    values = jax.random.normal(own_key, extent, jnp.float32) * scale * factor_of
    return jnp.minimum(jnp.maximum(values, -reach), reach).astype(kind)


def setup_inputs(seed: int = 0) -> dict:
    keys = jax.random.split(jax.random.key(seed), 13)
    latent = scatter_about(keys[0], (SEQ, D), 1.0, 6.0, ((0, 32),))
    context = scatter_about(keys[1], (CTX, D), 1.0, 6.0, ((0, 4),))
    condition = scatter_about(keys[2], (D,), 1.0, 6.0, (), jnp.float32)
    context_condition = scatter_about(keys[3], (D,), 1.0, 6.0, (), jnp.float32)
    modulation = scatter_about(keys[4], (3, D, D), D ** -0.5, 0.09375, ((1, 4), (2, 8)))
    query_weight = draw_query_weight(jax.random.fold_in(keys[12], 71), 0)
    key_weight = draw_key_weight(jax.random.fold_in(keys[12], 71), 0)
    value_weight = scatter_about(keys[7], (D, HEADS * HEAD_DIM), D ** -0.5, 0.09375, ((1, 8),))
    lambdas = jnp.clip(0.3 + 0.5 * jax.random.uniform(keys[8], (HEADS,), jnp.float32) ** steps_of(keys[8], (HEADS,), ((0, 8),), -0.2, 0.2), 0.3, 0.8)
    context_lift = jnp.clip(1.5 + 1.5 * jax.random.uniform(keys[9], (HEADS,), jnp.float32) ** steps_of(keys[9], (HEADS,), ((0, 8),), -0.2, 0.2), 1.5, 3.0)
    head_gain = jnp.clip(1.0 + 0.18 * jax.random.normal(keys[10], (HEAD_DIM,), jnp.float32), 0.1, 1.9)
    output_weight = scatter_about(keys[11], (HEADS * HEAD_DIM, D), (HEADS * HEAD_DIM) ** -0.5, 0.09375, ((0, 8),))
    return {"latent": latent, "context": context, "condition": condition, "context_condition": context_condition, "modulation": modulation, "query_weight": query_weight, "key_weight": key_weight, "value_weight": value_weight, "lambdas": lambdas, "context_lift": context_lift, "head_gain": head_gain, "output_weight": output_weight}


ROPE_BASE = 10000.0
EPSILON = 1e-05

def modulate(tokens_in, offset, scaling):
    values = tokens_in.astype(jnp.float32)
    center = lax.optimization_barrier(jnp.mean(values, axis=-1, keepdims=True))
    spread = lax.optimization_barrier(jnp.mean(jnp.square(values - center), axis=-1, keepdims=True))
    normed = (values - center) * lax.rsqrt(spread + EPSILON)
    return (normed * (1.0 + scaling) + offset).astype(jnp.bfloat16)

def rotate(tensor, places):
    number, head_count, head_width = tensor.shape
    quarter = head_width // 4
    eighth = head_width // 8
    inverse = ROPE_BASE ** (-jnp.arange(eighth, dtype=jnp.float32) / eighth)
    grid_row = (places // GRID_W).astype(jnp.float32)
    grid_col = (places % GRID_W).astype(jnp.float32)
    angles = jnp.stack([grid_row[:, None] * inverse, grid_col[:, None] * inverse], axis=1)
    cosine = jnp.cos(angles)[:, None, None, :, :]
    sine_table = jnp.sin(angles)[:, None, None, :, :]
    pieces = tensor.reshape(number, head_count, 2, 2, quarter)
    first_half = pieces[..., :eighth]
    second = pieces[..., eighth:]
    turned = jnp.concatenate([first_half * cosine - second * sine_table, second * cosine + first_half * sine_table], axis=-1)
    return turned.reshape(number, head_count, head_width)

def reference(latent, context, condition, context_condition, modulation, query_weight, key_weight, value_weight, lambdas, context_lift, head_gain, output_weight):
    silu_pair = jax.nn.silu(jnp.stack([condition, context_condition])).astype(jnp.bfloat16)
    mod_vectors = jnp.einsum('cd,rde->cre', silu_pair.astype(jnp.float32), modulation.astype(jnp.float32))
    normed = modulate(latent, mod_vectors[0, 0], mod_vectors[0, 1])
    normed_context = modulate(context, mod_vectors[1, 0], mod_vectors[1, 1])
    seq_len = latent.shape[0]
    half_width = HEAD_DIM // 2
    scale_factor = half_width ** (-0.5)
    query_raw = jnp.dot(normed, query_weight, preferred_element_type=jnp.float32).astype(jnp.bfloat16)
    key_raw = jnp.dot(normed, key_weight, preferred_element_type=jnp.float32).astype(jnp.bfloat16)
    latent_values = jnp.dot(normed, value_weight, preferred_element_type=jnp.float32).astype(jnp.bfloat16)
    context_keys = jnp.dot(normed_context, key_weight, preferred_element_type=jnp.float32).astype(jnp.bfloat16)
    context_values = jnp.dot(normed_context, value_weight, preferred_element_type=jnp.float32).astype(jnp.bfloat16)
    places = jnp.arange(seq_len, dtype=jnp.int32)
    queries = rotate(query_raw.astype(jnp.float32).reshape(seq_len, HEADS, HEAD_DIM), places).astype(jnp.bfloat16)
    latent_keys = rotate(key_raw.astype(jnp.float32).reshape(seq_len, HEADS, HEAD_DIM), places).astype(jnp.bfloat16)
    all_keys = jnp.concatenate([context_keys.reshape(CTX, HEADS, HEAD_DIM), latent_keys], axis=0)
    all_values = jnp.concatenate([context_values.reshape(CTX, HEADS, HEAD_DIM), latent_values.reshape(seq_len, HEADS, HEAD_DIM)], axis=0)
    key_total = CTX + seq_len
    block_len = math.gcd(seq_len, 1024)

    def one_head(inputs):
        head_queries, head_keys, head_values, head_lambda, head_lift = inputs
        lift_row = jnp.where(jnp.arange(key_total) < CTX, head_lift, 0.0)

        def one_block(block_queries):
            outputs = []
            for map_index in range(2):
                low_col = map_index * half_width
                scores = jnp.dot(block_queries[:, low_col:low_col + half_width], head_keys[:, low_col:low_col + half_width].T, preferred_element_type=jnp.float32) * scale_factor + lift_row
                row_peak = lax.optimization_barrier(jnp.max(scores, axis=1, keepdims=True))
                weights = jnp.exp(scores - row_peak)
                row_sums = lax.optimization_barrier(jnp.sum(weights, axis=1, keepdims=True))
                outputs.append(jnp.dot(weights.astype(jnp.bfloat16), head_values, preferred_element_type=jnp.float32) / row_sums)
            difference = outputs[0] - head_lambda * outputs[1]
            scaled = difference * lax.rsqrt(lax.optimization_barrier(jnp.mean(jnp.square(difference), axis=1, keepdims=True)) + EPSILON) * head_gain
            return scaled.astype(jnp.bfloat16)
        blocks = head_queries.reshape(seq_len // block_len, block_len, HEAD_DIM)
        return lax.map(one_block, blocks).reshape(seq_len, HEAD_DIM)
    heads_out = lax.map(one_head, (queries.transpose(1, 0, 2), all_keys.transpose(1, 0, 2), all_values.transpose(1, 0, 2), lambdas, context_lift))
    attended = heads_out.transpose(1, 0, 2).reshape(seq_len, HEADS * HEAD_DIM)
    mixture = jnp.dot(attended, output_weight, preferred_element_type=jnp.float32)
    return (latent.astype(jnp.float32) + mod_vectors[0, 2] * mixture).astype(jnp.bfloat16)
```

```python
import functools

import jax
import jax.numpy as jnp
from jax import lax
from jax.experimental import pallas as pl
from jax.experimental.pallas import tpu as pltpu
from jax.sharding import PartitionSpec as P

GRID_W = 64
ROPE_BASE = 10000.0
EPSILON = 1e-05
LOG2E = 1.4426950408889634
ROWS = 16
VMEM_LIMIT = 62 * 1024 * 1024
MESH = pl.DeviceIdType.MESH


def remote(src, dst, send_sem, recv_sem, **where):
    return pltpu.make_async_remote_copy(
        src_ref=src,
        dst_ref=dst,
        send_sem=send_sem,
        recv_sem=recv_sem,
        device_id=where,
        device_id_type=MESH,
    )


def aligned(start, size, unit):
    return pl.ds(pl.multiple_of(start, unit), size)


def attend_kernel(
    sp_size,
    tp_size,
    latent,
    context,
    condition,
    context_condition,
    modulation,
    query_weight,
    key_weight,
    value_weight,
    cosine,
    sine,
    lambdas,
    lift,
    gain,
    attended,
    gate,
    tokens,
    context_tokens,
    normed,
    mod_weight,
    wq,
    wk,
    wv,
    keys_values,
    queries,
    mod_parts,
    mod_pieces,
    mod_rows,
    local_sem,
    tok_send,
    tok_recv,
    part_send,
    part_recv,
    piece_send,
    piece_recv,
    kv_send,
    kv_recv,
):
    s = lax.axis_index("sp")
    t = lax.axis_index("tp")
    z = lax.div(t, 2)
    c = lax.rem(t, 2)
    chips = tp_size // 2
    rows, width = latent.shape
    pair = 2 * rows
    block_tokens = tp_size * rows
    ctx_rows = context.shape[0]
    ctx_total = ctx_rows * sp_size
    local = query_weight.shape[1]
    heads = lambdas.shape[0]
    head = local // heads
    half = head // 2
    piece = modulation.shape[2]
    depth = modulation.shape[1]

    own_slot = tokens.at[aligned(t * rows, rows, ROWS)]
    locals_ = [
        pltpu.make_async_copy(src, dst, local_sem.at[i])
        for i, (src, dst) in enumerate(
            [
                (modulation, mod_weight),
                (latent, own_slot),
                (context, context_tokens),
                (key_weight, wk),
                (value_weight, wv),
                (query_weight, wq),
            ]
        )
    ]
    for copy in locals_:
        copy.start()

    barrier = pltpu.get_barrier_semaphore()
    for k in range(1, tp_size):
        pl.semaphore_signal(
            barrier, inc=1, device_id={"tp": lax.rem(t + k, tp_size)}, device_id_type=MESH
        )
    for k in range(1, sp_size):
        pl.semaphore_signal(
            barrier, inc=1, device_id={"sp": lax.rem(s + k, sp_size)}, device_id_type=MESH
        )
    pl.semaphore_wait(barrier, tp_size + sp_size - 2)

    def token_copy(kind, b, core, src=None):
        slot = 2 * b + core
        place = tokens.at[aligned(slot * rows, rows, ROWS)]
        to = (t + 2, t - 2, t + 1 - 2 * c)[kind]
        return remote(
            place if src is None else src,
            place,
            tok_send.at[kind, b],
            tok_recv.at[slot],
            tp=to,
        )

    @pl.when(z + 1 < chips)
    def _():
        token_copy(0, z, c, latent).start()

    @pl.when(z > 0)
    def _():
        token_copy(1, z, c, latent).start()

    token_copy(2, z, c, latent).start()

    def silu(ref):
        v = ref[:, aligned(s * depth, depth, 128)]
        return v / (1.0 + jnp.exp(-v))

    first = silu(condition)
    second = silu(context_condition)
    which = lax.broadcasted_iota(jnp.int32, (ROWS, depth), 0)
    vectors = jnp.where(
        which == 0, jnp.broadcast_to(first, (ROWS, depth)), jnp.broadcast_to(second, (ROWS, depth))
    ).astype(jnp.bfloat16)
    locals_[0].wait()
    for r in range(3):
        found = jnp.dot(vectors, mod_weight[r], preferred_element_type=jnp.float32)
        mod_parts[s, 2 * r : 2 * r + 2, :] = found[0:2]
    mod_parts[s, 6:8, :] = jnp.zeros((2, piece), jnp.float32)

    def part_copy(k, owner):
        return remote(
            mod_parts.at[owner],
            mod_parts.at[owner],
            part_send.at[k],
            part_recv.at[owner],
            sp=lax.rem(s + k, sp_size),
        )

    def piece_copy(k, owner):
        return remote(
            mod_pieces.at[owner],
            mod_pieces.at[owner],
            piece_send.at[k],
            piece_recv.at[owner],
            tp=lax.rem(t + k, tp_size),
        )

    for k in range(1, sp_size):
        part_copy(k, s).start()
    for k in range(1, sp_size):
        part_copy(k, lax.rem(s + k, sp_size)).wait_recv()
    total = mod_parts[0]
    for i in range(1, sp_size):
        total = total + mod_parts[i]
    mod_pieces[t] = total
    for k in range(1, tp_size):
        piece_copy(k, t).start()

    def forward(d):
        left = z - d
        right = z + d

        @pl.when(left >= 0)
        def _():
            token_copy(2, left, c).wait_recv()

            @pl.when(z + 1 < chips)
            def _():
                token_copy(0, left, c).start()

            token_copy(2, left, c).start()

        @pl.when(right < chips)
        def _():
            token_copy(2, right, c).wait_recv()

            @pl.when(z > 0)
            def _():
                token_copy(1, right, c).start()

            token_copy(2, right, c).start()

    forward(1)
    for k in range(1, tp_size):
        piece_copy(k, lax.rem(t + k, tp_size)).wait_recv()
    for i in range(tp_size):
        mod_rows[:, i * piece : (i + 1) * piece] = mod_pieces[i]
    gate[...] = mod_rows[4:5, :]

    def normalise(source, base, count, row):
        def group(i, carry):
            x = source[aligned(base + i * ROWS, ROWS, ROWS), :].astype(jnp.float32)
            x = x - jnp.sum(x, axis=1, keepdims=True) * (1.0 / width)
            spread = jnp.sum(x * x, axis=1, keepdims=True) * (1.0 / width)
            y = x * lax.rsqrt(spread + EPSILON)
            y = y * (1.0 + mod_rows[2 + row : 3 + row, :]) + mod_rows[row : row + 1, :]
            normed[aligned(i * ROWS, ROWS, ROWS), :] = y.astype(jnp.bfloat16)
            return carry

        lax.fori_loop(0, count // ROWS, group, 0)

    def kv_copy(k, owner, b, is_context):
        if is_context:
            place = keys_values.at[aligned(owner * ctx_rows, ctx_rows, ROWS)]
        else:
            place = keys_values.at[
                aligned(ctx_total + owner * block_tokens + b * pair, pair, ROWS)
            ]
        return remote(
            place, place, kv_send.at[k, b], kv_recv.at[owner, b], sp=lax.rem(s + k, sp_size)
        )

    locals_[1].wait()
    locals_[2].wait()
    normalise(context_tokens, 0, ctx_rows, 1)
    locals_[3].wait()
    locals_[4].wait()
    ctx_place = aligned(s * ctx_rows, ctx_rows, ROWS)
    keys_values[ctx_place, :local] = jnp.dot(
        normed[:ctx_rows, :], wk[...], preferred_element_type=jnp.float32
    ).astype(jnp.bfloat16)
    keys_values[ctx_place, local:] = jnp.dot(
        normed[:ctx_rows, :], wv[...], preferred_element_type=jnp.float32
    ).astype(jnp.bfloat16)
    for k in range(1, sp_size):
        kv_copy(k, s, chips, True).start()
    locals_[5].wait()

    quarter = half // 4
    lane = lax.broadcasted_iota(jnp.int32, (pair, half), 1)
    low = lax.rem(lane, 2 * quarter) < quarter

    def turn(raw, b):
        cos = cosine[aligned(b * pair, pair, ROWS), :]
        sin = sine[aligned(b * pair, pair, ROWS), :]
        parts = []
        for i in range(local // half):
            v = raw[:, i * half : (i + 1) * half].astype(jnp.bfloat16).astype(jnp.float32)
            other = jnp.where(low, pltpu.roll(v, half - quarter, 1), pltpu.roll(v, quarter, 1))
            parts.append((v * cos + other * sin).astype(jnp.bfloat16))
        return jnp.concatenate(parts, axis=1)

    def process(b):
        token_copy(2, b, 1 - c).wait_recv()
        normalise(tokens, b * pair, pair, 0)
        place = aligned(ctx_total + s * block_tokens + b * pair, pair, ROWS)
        x = normed[:pair, :]
        keys_values[place, :local] = turn(
            jnp.dot(x, wk[...], preferred_element_type=jnp.float32), b
        )
        keys_values[place, local:] = jnp.dot(
            x, wv[...], preferred_element_type=jnp.float32
        ).astype(jnp.bfloat16)
        for k in range(1, sp_size):
            kv_copy(k, s, b, False).start()
        queries[aligned(b * pair, pair, ROWS), :] = turn(
            jnp.dot(x, wq[...], preferred_element_type=jnp.float32), b
        )

    def step(j, carry):
        d = lax.div(j, 2)
        side = lax.rem(j, 2)

        @pl.when((side == 0) & (d >= 1) & (d + 1 < chips))
        def _():
            forward(d + 1)

        b = z - d + 2 * d * side

        @pl.when((b >= 0) & (b < chips) & (d + 1 > side))
        def _():
            process(b)

        return carry

    lax.fori_loop(0, 2 * chips, step, 0)

    for k in range(1, sp_size):
        owner = lax.rem(s + k, sp_size)
        kv_copy(k, owner, chips, True).wait_recv()
        for b in range(chips):
            kv_copy(k, owner, b, False).wait_recv()

    tile = min(256, block_tokens)
    key_total = keys_values.shape[0]
    factor = half ** (-0.5) * LOG2E
    on_context = lax.broadcasted_iota(jnp.int32, (1, key_total), 1) < ctx_total

    def attention(i, carry):
        place = aligned(i * tile, tile, ROWS)
        for h in range(heads):
            raised = jnp.where(on_context, lift[h] * LOG2E, 0.0)
            value = keys_values[:, local + h * head : local + (h + 1) * head]
            outs = []
            for m in range(2):
                at = h * head + m * half
                scores = lax.dot_general(
                    queries[place, at : at + half],
                    keys_values[:, at : at + half],
                    (((1,), (1,)), ((), ())),
                    preferred_element_type=jnp.float32,
                )
                scores = scores * factor + raised
                weights = jnp.exp2(scores - jnp.max(scores, axis=1, keepdims=True))
                sums = jnp.sum(weights, axis=1, keepdims=True)
                outs.append(
                    jnp.dot(
                        weights.astype(jnp.bfloat16), value, preferred_element_type=jnp.float32
                    )
                    / sums
                )
            diff = outs[0] - lambdas[h] * outs[1]
            mean = jnp.sum(diff * diff, axis=1, keepdims=True) * (1.0 / head)
            attended[place, h * head : (h + 1) * head] = (
                diff * lax.rsqrt(mean + EPSILON) * gain[...]
            ).astype(jnp.bfloat16)
        return carry

    lax.fori_loop(0, block_tokens // tile, attention, 0)

    for b in range(chips):

        @pl.when((b <= z) & (z + 1 < chips))
        def _():
            token_copy(0, b, c).wait_send()

        @pl.when((b >= z) & (z > 0))
        def _():
            token_copy(1, b, c).wait_send()

        token_copy(2, b, c).wait_send()
    for k in range(1, tp_size):
        piece_copy(k, t).wait_send()
    for k in range(1, sp_size):
        part_copy(k, s).wait_send()
        kv_copy(k, s, chips, True).wait_send()
        for b in range(chips):
            kv_copy(k, s, b, False).wait_send()


def output_kernel(
    tp_size,
    attended,
    output_weight,
    latent,
    gate,
    result,
    weight,
    own,
    pair_send,
    pair_recv,
    stage,
    from_left,
    from_right,
    local_sem,
    ps_sem,
    pr_sem,
    st_sem,
    left_sem,
    right_sem,
):
    t = lax.axis_index("tp")
    z = lax.div(t, 2)
    c = lax.rem(t, 2)
    chips = tp_size // 2
    rows, width = latent.shape
    chunk = min(1024, width)

    load = pltpu.make_async_copy(output_weight, weight, local_sem)
    load.start()
    barrier = pltpu.get_barrier_semaphore()

    @pl.when(z > 0)
    def _():
        pl.semaphore_signal(barrier, inc=1, device_id={"tp": t - 2}, device_id_type=MESH)

    @pl.when(z + 1 < chips)
    def _():
        pl.semaphore_signal(barrier, inc=1, device_id={"tp": t + 2}, device_id_type=MESH)

    pl.semaphore_signal(barrier, inc=1, device_id={"tp": t + 1 - 2 * c}, device_id_type=MESH)
    inner = (z > 0) & (z + 1 < chips)
    pl.semaphore_wait(barrier, jnp.where(inner, 3, 2) if chips > 1 else 1)

    load.wait()

    def pair_copy(b):
        return remote(
            pair_send.at[b], pair_recv.at[b], ps_sem.at[b], pr_sem.at[b], tp=t + 1 - 2 * c
        )

    def right_copy(b):
        return remote(stage.at[b], from_left.at[b], st_sem.at[b], left_sem.at[b], tp=t + 2)

    def left_copy(b):
        return remote(stage.at[b], from_right.at[b], st_sem.at[b], right_sem.at[b], tp=t - 2)

    def compute(b):
        other = attended[aligned((2 * b + 1 - c) * rows, rows, ROWS), :]
        mine = attended[aligned((2 * b + c) * rows, rows, ROWS), :]
        both = jnp.concatenate([other, mine], axis=0)
        for n in range(width // chunk):
            cols = slice(n * chunk, (n + 1) * chunk)
            found = jnp.dot(both, weight[:, cols], preferred_element_type=jnp.float32)
            pair_send[b, :, cols] = found[:rows].astype(jnp.bfloat16)
            own[b, :, cols] = found[rows:]
        pair_copy(b).start()

    def combine(b):
        pair_copy(b).wait_recv()

        @pl.when(b > z)
        def _():
            @pl.when(z > 0)
            def _():
                right_copy(b).wait_recv()
                stage[b] = (
                    own[b] + pair_recv[b].astype(jnp.float32) + from_left[b].astype(jnp.float32)
                ).astype(jnp.bfloat16)

            @pl.when(z == 0)
            def _():
                stage[b] = (own[b] + pair_recv[b].astype(jnp.float32)).astype(jnp.bfloat16)

            right_copy(b).start()

        @pl.when(b < z)
        def _():
            @pl.when(z + 1 < chips)
            def _():
                left_copy(b).wait_recv()
                stage[b] = (
                    own[b] + pair_recv[b].astype(jnp.float32) + from_right[b].astype(jnp.float32)
                ).astype(jnp.bfloat16)

            @pl.when(z + 1 == chips)
            def _():
                stage[b] = (own[b] + pair_recv[b].astype(jnp.float32)).astype(jnp.bfloat16)

            left_copy(b).start()

    def place_of(j):
        d = chips - 1 - lax.div(j, 2)
        side = lax.rem(j, 2)
        b = z - d + 2 * d * side
        return b, (b >= 0) & (b < chips) & (d + 1 > side)

    at_end = (z == 0) | (z + 1 == chips)

    def first_pass(j, carry):
        b, valid = place_of(j)

        @pl.when(valid)
        def _():
            compute(b)

            @pl.when(at_end & (b != z))
            def _():
                combine(b)

        return carry

    lax.fori_loop(0, 2 * chips, first_pass, 0)

    def second_pass(j, carry):
        b, valid = place_of(j)

        @pl.when(valid & jnp.logical_not(at_end) & (b != z))
        def _():
            combine(b)

        return carry

    lax.fori_loop(0, 2 * chips, second_pass, 0)

    pair_copy(z).wait_recv()
    own[z] = own[z] + pair_recv[z].astype(jnp.float32)

    @pl.when(z > 0)
    def _():
        right_copy(z).wait_recv()
        own[z] = own[z] + from_left[z].astype(jnp.float32)

    @pl.when(z + 1 < chips)
    def _():
        left_copy(z).wait_recv()
        own[z] = own[z] + from_right[z].astype(jnp.float32)

    result[...] = (latent[...].astype(jnp.float32) + gate[...] * own[z]).astype(jnp.bfloat16)

    for b in range(chips):
        pair_copy(b).wait_send()

        @pl.when(b > z)
        def _():
            right_copy(b).wait_send()

        @pl.when(b < z)
        def _():
            left_copy(b).wait_send()


def tables(places, half):
    quarter = half // 4
    inverse = ROPE_BASE ** (-jnp.arange(quarter, dtype=jnp.float32) / quarter)
    by_row = (places // GRID_W).astype(jnp.float32)[:, None] * inverse
    by_col = (places % GRID_W).astype(jnp.float32)[:, None] * inverse
    angles = jnp.concatenate([by_row, by_row, by_col, by_col], axis=1)
    sign = jnp.where(jnp.arange(half) % (2 * quarter) < quarter, -1.0, 1.0)
    return jnp.cos(angles), jnp.sin(angles) * sign


def shards(
    sp_size,
    tp_size,
    latent,
    context,
    condition,
    context_condition,
    modulation,
    query_weight,
    key_weight,
    value_weight,
    lambdas,
    context_lift,
    head_gain,
    output_weight,
):
    rows, width = latent.shape
    chips = tp_size // 2
    local = query_weight.shape[1]
    half = local // lambdas.shape[0] // 2
    block_tokens = rows * tp_size
    ctx_rows = context.shape[0]
    piece = modulation.shape[2]
    places = lax.axis_index("sp") * block_tokens + jnp.arange(block_tokens, dtype=jnp.int32)
    cosine, sine = tables(places, half)
    vmem = pl.BlockSpec(memory_space=pltpu.VMEM)
    smem = pl.BlockSpec(memory_space=pltpu.SMEM)
    anywhere = pl.BlockSpec(memory_space=pl.ANY)
    bf16, f32 = jnp.bfloat16, jnp.float32
    dma = pltpu.SemaphoreType.DMA
    attended, gate = pl.pallas_call(
        functools.partial(attend_kernel, sp_size, tp_size),
        out_shape=(
            jax.ShapeDtypeStruct((block_tokens, local), bf16),
            jax.ShapeDtypeStruct((1, width), f32),
        ),
        in_specs=[anywhere] * 2 + [vmem] * 2 + [anywhere] * 4 + [vmem] * 2 + [smem] * 2 + [vmem],
        out_specs=(vmem, vmem),
        scratch_shapes=[
            pltpu.VMEM((block_tokens, width), bf16),
            pltpu.VMEM(context.shape, bf16),
            pltpu.VMEM((max(2 * rows, ctx_rows), width), bf16),
            pltpu.VMEM(modulation.shape, bf16),
            pltpu.VMEM((width, local), bf16),
            pltpu.VMEM((width, local), bf16),
            pltpu.VMEM((width, local), bf16),
            pltpu.VMEM((sp_size * (ctx_rows + block_tokens), 2 * local), bf16),
            pltpu.VMEM((block_tokens, local), bf16),
            pltpu.VMEM((sp_size, 8, piece), f32),
            pltpu.VMEM((tp_size, 8, piece), f32),
            pltpu.VMEM((8, width), f32),
            dma((6,)),
            dma((3, chips)),
            dma((tp_size,)),
            dma((sp_size,)),
            dma((sp_size,)),
            dma((tp_size,)),
            dma((tp_size,)),
            dma((sp_size, chips + 1)),
            dma((sp_size, chips + 1)),
        ],
        compiler_params=pltpu.CompilerParams(
            collective_id=0, has_side_effects=True, vmem_limit_bytes=VMEM_LIMIT
        ),
        name="attend",
    )(
        latent,
        context,
        condition.reshape(1, -1),
        context_condition.reshape(1, -1),
        modulation,
        query_weight,
        key_weight,
        value_weight,
        cosine,
        sine,
        lambdas,
        context_lift,
        head_gain.reshape(1, -1),
    )
    blocks = (chips, rows, width)
    return pl.pallas_call(
        functools.partial(output_kernel, tp_size),
        out_shape=jax.ShapeDtypeStruct((rows, width), bf16),
        in_specs=[vmem, anywhere, vmem, vmem],
        out_specs=vmem,
        scratch_shapes=[
            pltpu.VMEM(output_weight.shape, bf16),
            pltpu.VMEM(blocks, f32),
            pltpu.VMEM(blocks, bf16),
            pltpu.VMEM(blocks, bf16),
            pltpu.VMEM(blocks, bf16),
            pltpu.VMEM(blocks, bf16),
            pltpu.VMEM(blocks, bf16),
            dma(()),
            dma((chips,)),
            dma((chips,)),
            dma((chips,)),
            dma((chips,)),
            dma((chips,)),
        ],
        compiler_params=pltpu.CompilerParams(
            collective_id=1, has_side_effects=True, vmem_limit_bytes=VMEM_LIMIT
        ),
        name="output",
    )(attended, output_weight, latent, gate)


def solution(mesh):
    in_specs = (
        P(("sp", "tp"), None),
        P("sp", None),
        P(),
        P(),
        P(None, "sp", "tp"),
        P(None, "tp"),
        P(None, "tp"),
        P(None, "tp"),
        P("tp"),
        P("tp"),
        P(),
        P("tp", None),
    )
    out_specs = P(("sp", "tp"), None)
    body = functools.partial(shards, mesh.shape["sp"], mesh.shape["tp"])
    return jax.shard_map(body, mesh=mesh, in_specs=in_specs, out_specs=out_specs, check_vma=False)
```

```python
import functools

import jax
import jax.numpy as jnp
from jax import lax
from jax.experimental import pallas as pl
from jax.experimental.pallas import tpu as pltpu
from jax.sharding import PartitionSpec as P

GRID_W = 64
ROPE_BASE = 10000.0
EPSILON = 1e-05
LOG2E = 1.4426950408889634
ROWS = 16
VMEM_LIMIT = 62 * 1024 * 1024
MESH = pl.DeviceIdType.MESH


def remote(src, dst, send_sem, recv_sem, **where):
    return pltpu.make_async_remote_copy(
        src_ref=src,
        dst_ref=dst,
        send_sem=send_sem,
        recv_sem=recv_sem,
        device_id=where,
        device_id_type=MESH,
    )


def aligned(start, size, unit):
    return pl.ds(pl.multiple_of(start, unit), size)


def attend_kernel(
    sp_size,
    tp_size,
    latent,
    context,
    condition,
    context_condition,
    modulation,
    query_weight,
    key_weight,
    value_weight,
    cosine,
    sine,
    lambdas,
    lift,
    gain,
    attended,
    gate,
    tokens,
    context_tokens,
    normed,
    mod_weight,
    wq,
    wk,
    wv,
    keys_values,
    queries,
    kv_stage,
    q_stage,
    out_stage,
    mod_parts,
    mod_pieces,
    mod_rows,
    local_sem,
    tok_send,
    tok_recv,
    part_send,
    part_recv,
    piece_send,
    piece_recv,
    kv_send,
    kv_recv,
    q_send,
    q_recv,
    out_send,
    out_recv,
):
    s = lax.axis_index("sp")
    t = lax.axis_index("tp")
    z = lax.div(t, 2)
    c = lax.rem(t, 2)
    chips = tp_size // 2
    rows, width = latent.shape
    pair = 2 * rows
    block_tokens = tp_size * rows
    ctx_rows = context.shape[0]
    ctx_total = ctx_rows * sp_size
    local = query_weight.shape[1]
    heads = lambdas.shape[0]
    head = local // heads
    half = head // 2
    piece = modulation.shape[2]
    depth = modulation.shape[1]

    own_slot = tokens.at[aligned(t * rows, rows, ROWS)]
    locals_ = [
        pltpu.make_async_copy(src, dst, local_sem.at[i])
        for i, (src, dst) in enumerate(
            [
                (modulation, mod_weight),
                (latent, own_slot),
                (context, context_tokens),
                (key_weight, wk),
                (value_weight, wv),
                (query_weight, wq),
            ]
        )
    ]
    for copy in locals_:
        copy.start()

    barrier = pltpu.get_barrier_semaphore()
    for k in range(1, tp_size):
        pl.semaphore_signal(
            barrier, inc=1, device_id={"tp": lax.rem(t + k, tp_size)}, device_id_type=MESH
        )
    for k in range(1, sp_size):
        pl.semaphore_signal(
            barrier, inc=1, device_id={"sp": lax.rem(s + k, sp_size)}, device_id_type=MESH
        )
    pl.semaphore_wait(barrier, tp_size + sp_size - 2)

    def token_copy(kind, b, core, src=None):
        slot = 2 * b + core
        place = tokens.at[aligned(slot * rows, rows, ROWS)]
        to = (t + 2, t - 2, t + 1 - 2 * c)[kind]
        return remote(
            place if src is None else src,
            place,
            tok_send.at[kind, b],
            tok_recv.at[slot],
            tp=to,
        )

    @pl.when(z + 1 < chips)
    def _():
        token_copy(0, z, c, latent).start()

    @pl.when(z > 0)
    def _():
        token_copy(1, z, c, latent).start()

    token_copy(2, z, c, latent).start()

    def silu(ref):
        v = ref[:, aligned(s * depth, depth, 128)]
        return v / (1.0 + jnp.exp(-v))

    first = silu(condition)
    second = silu(context_condition)
    which = lax.broadcasted_iota(jnp.int32, (ROWS, depth), 0)
    vectors = jnp.where(
        which == 0, jnp.broadcast_to(first, (ROWS, depth)), jnp.broadcast_to(second, (ROWS, depth))
    ).astype(jnp.bfloat16)
    locals_[0].wait()
    for r in range(3):
        found = jnp.dot(vectors, mod_weight[r], preferred_element_type=jnp.float32)
        mod_parts[s, 2 * r : 2 * r + 2, :] = found[0:2]
    mod_parts[s, 6:8, :] = jnp.zeros((2, piece), jnp.float32)

    def part_copy(k, owner):
        return remote(
            mod_parts.at[owner],
            mod_parts.at[owner],
            part_send.at[k],
            part_recv.at[owner],
            sp=lax.rem(s + k, sp_size),
        )

    def piece_copy(k, owner):
        return remote(
            mod_pieces.at[owner],
            mod_pieces.at[owner],
            piece_send.at[k],
            piece_recv.at[owner],
            tp=lax.rem(t + k, tp_size),
        )

    for k in range(1, sp_size):
        part_copy(k, s).start()
    for k in range(1, sp_size):
        part_copy(k, lax.rem(s + k, sp_size)).wait_recv()
    total = mod_parts[0]
    for i in range(1, sp_size):
        total = total + mod_parts[i]
    mod_pieces[t] = total
    for k in range(1, tp_size):
        piece_copy(k, t).start()

    def forward(d):
        left = z - d
        right = z + d

        @pl.when(left >= 0)
        def _():
            token_copy(2, left, c).wait_recv()

            @pl.when(z + 1 < chips)
            def _():
                token_copy(0, left, c).start()

            token_copy(2, left, c).start()

        @pl.when(right < chips)
        def _():
            token_copy(2, right, c).wait_recv()

            @pl.when(z > 0)
            def _():
                token_copy(1, right, c).start()

            token_copy(2, right, c).start()

    forward(1)
    for k in range(1, tp_size):
        piece_copy(k, lax.rem(t + k, tp_size)).wait_recv()
    for i in range(tp_size):
        mod_rows[:, i * piece : (i + 1) * piece] = mod_pieces[i]
    gate[...] = mod_rows[4:5, :]

    def normalise(source, base, count, row):
        def group(i, carry):
            x = source[aligned(base + i * ROWS, ROWS, ROWS), :].astype(jnp.float32)
            x = x - jnp.sum(x, axis=1, keepdims=True) * (1.0 / width)
            spread = jnp.sum(x * x, axis=1, keepdims=True) * (1.0 / width)
            y = x * lax.rsqrt(spread + EPSILON)
            y = y * (1.0 + mod_rows[2 + row : 3 + row, :]) + mod_rows[row : row + 1, :]
            normed[aligned(i * ROWS, ROWS, ROWS), :] = y.astype(jnp.bfloat16)
            return carry

        lax.fori_loop(0, count // ROWS, group, 0)

    my_head = lax.rem(s, heads)

    def mate(k):
        return lax.rem(my_head + k, heads)

    def kv_place(owner, b, is_context):
        if is_context:
            return aligned(owner * ctx_rows, ctx_rows, ROWS)
        return aligned(ctx_total + owner * block_tokens + b * pair, pair, ROWS)

    def stage_place(b, is_context):
        if is_context:
            return aligned(block_tokens, ctx_rows, ROWS)
        return aligned(b * pair, pair, ROWS)

    def kv_copy(k, owner, b, is_context):
        to = lax.rem(s + k, sp_size)
        return remote(
            kv_stage.at[lax.rem(to, heads), stage_place(b, is_context)],
            keys_values.at[kv_place(owner, b, is_context)],
            kv_send.at[k, b],
            kv_recv.at[owner, b],
            sp=to,
        )

    def q_copy(k, slot, b):
        place = aligned(b * pair, pair, ROWS)
        return remote(
            q_stage.at[mate(k), place],
            queries.at[slot, place],
            q_send.at[k, b],
            q_recv.at[slot, b],
            sp=s - my_head + mate(k),
        )

    def out_copy(k, head_index):
        return remote(
            out_stage.at[mate(k)],
            attended.at[head_index],
            out_send.at[k],
            out_recv.at[head_index],
            sp=s - my_head + mate(k),
        )

    def hand_out(keys, values, b, is_context):
        place = stage_place(b, is_context)
        for g in range(heads):
            kv_stage[g, place, :head] = keys[:, g * head : (g + 1) * head]
            kv_stage[g, place, head:] = values[:, g * head : (g + 1) * head]
        for k in range(1, sp_size):
            kv_copy(k, s, b, is_context).start()
        keys_values[kv_place(s, b, is_context), :] = kv_stage[my_head, place, :]

    locals_[1].wait()
    locals_[2].wait()
    normalise(context_tokens, 0, ctx_rows, 1)
    locals_[3].wait()
    locals_[4].wait()
    hand_out(
        jnp.dot(normed[:ctx_rows, :], wk[...], preferred_element_type=jnp.float32).astype(
            jnp.bfloat16
        ),
        jnp.dot(normed[:ctx_rows, :], wv[...], preferred_element_type=jnp.float32).astype(
            jnp.bfloat16
        ),
        chips,
        True,
    )
    locals_[5].wait()

    quarter = half // 4
    lane = lax.broadcasted_iota(jnp.int32, (pair, half), 1)
    low = lax.rem(lane, 2 * quarter) < quarter

    def turn(raw, b):
        cos = cosine[aligned(b * pair, pair, ROWS), :]
        sin = sine[aligned(b * pair, pair, ROWS), :]
        parts = []
        for i in range(local // half):
            v = raw[:, i * half : (i + 1) * half].astype(jnp.bfloat16).astype(jnp.float32)
            other = jnp.where(low, pltpu.roll(v, half - quarter, 1), pltpu.roll(v, quarter, 1))
            parts.append((v * cos + other * sin).astype(jnp.bfloat16))
        return jnp.concatenate(parts, axis=1)

    def process(b):
        token_copy(2, b, 1 - c).wait_recv()
        normalise(tokens, b * pair, pair, 0)
        x = normed[:pair, :]
        hand_out(
            turn(jnp.dot(x, wk[...], preferred_element_type=jnp.float32), b),
            jnp.dot(x, wv[...], preferred_element_type=jnp.float32).astype(jnp.bfloat16),
            b,
            False,
        )
        turned = turn(jnp.dot(x, wq[...], preferred_element_type=jnp.float32), b)
        place = aligned(b * pair, pair, ROWS)
        for g in range(heads):
            q_stage[g, place, :] = turned[:, g * head : (g + 1) * head]
        for k in range(1, heads):
            q_copy(k, my_head, b).start()
        queries[my_head, place, :] = q_stage[my_head, place, :]

    def step(j, carry):
        d = lax.div(j, 2)
        side = lax.rem(j, 2)

        @pl.when((side == 0) & (d >= 1) & (d + 1 < chips))
        def _():
            forward(d + 1)

        b = z - d + 2 * d * side

        @pl.when((b >= 0) & (b < chips) & (d + 1 > side))
        def _():
            process(b)

        return carry

    lax.fori_loop(0, 2 * chips, step, 0)

    for k in range(1, sp_size):
        owner = lax.rem(s + k, sp_size)
        kv_copy(k, owner, chips, True).wait_recv()
        for b in range(chips):
            kv_copy(k, owner, b, False).wait_recv()
    for k in range(1, heads):
        for b in range(chips):
            q_copy(k, mate(k), b).wait_recv()

    tile = min(256, block_tokens)
    key_total = keys_values.shape[0]
    factor = half ** (-0.5) * LOG2E
    on_context = lax.broadcasted_iota(jnp.int32, (1, key_total), 1) < ctx_total

    raised = jnp.where(on_context, lift[my_head] * LOG2E, 0.0)
    weight_of_second = lambdas[my_head]

    def attention(i, slot):
        place = aligned(i * tile, tile, ROWS)
        outs = []
        for m in range(2):
            scores = lax.dot_general(
                queries[slot, place, m * half : (m + 1) * half],
                keys_values[:, m * half : (m + 1) * half],
                (((1,), (1,)), ((), ())),
                preferred_element_type=jnp.float32,
            )
            scores = scores * factor + raised
            weights = jnp.exp2(scores - jnp.max(scores, axis=1, keepdims=True))
            sums = jnp.sum(weights, axis=1, keepdims=True)
            outs.append(
                jnp.dot(
                    weights.astype(jnp.bfloat16),
                    keys_values[:, head:],
                    preferred_element_type=jnp.float32,
                )
                / sums
            )
        diff = outs[0] - weight_of_second * outs[1]
        mean = jnp.sum(diff * diff, axis=1, keepdims=True) * (1.0 / head)
        out_stage[slot, place, :] = (diff * lax.rsqrt(mean + EPSILON) * gain[...]).astype(
            jnp.bfloat16
        )
        return slot

    for k in range(1, heads + 1):
        lax.fori_loop(0, block_tokens // tile, attention, mate(k))
        if k < heads:
            out_copy(k, my_head).start()
    attended[my_head] = out_stage[my_head]
    for k in range(1, heads):
        out_copy(k, mate(k)).wait_recv()
        out_copy(k, my_head).wait_send()
        for b in range(chips):
            q_copy(k, my_head, b).wait_send()

    for b in range(chips):

        @pl.when((b <= z) & (z + 1 < chips))
        def _():
            token_copy(0, b, c).wait_send()

        @pl.when((b >= z) & (z > 0))
        def _():
            token_copy(1, b, c).wait_send()

        token_copy(2, b, c).wait_send()
    for k in range(1, tp_size):
        piece_copy(k, t).wait_send()
    for k in range(1, sp_size):
        part_copy(k, s).wait_send()
        kv_copy(k, s, chips, True).wait_send()
        for b in range(chips):
            kv_copy(k, s, b, False).wait_send()


def output_kernel(
    tp_size,
    attended,
    output_weight,
    latent,
    gate,
    result,
    weight,
    own,
    pair_send,
    pair_recv,
    stage,
    from_left,
    from_right,
    local_sem,
    ps_sem,
    pr_sem,
    st_sem,
    left_sem,
    right_sem,
):
    t = lax.axis_index("tp")
    z = lax.div(t, 2)
    c = lax.rem(t, 2)
    chips = tp_size // 2
    rows, width = latent.shape
    chunk = min(1024, width)

    load = pltpu.make_async_copy(output_weight, weight, local_sem)
    load.start()
    barrier = pltpu.get_barrier_semaphore()

    @pl.when(z > 0)
    def _():
        pl.semaphore_signal(barrier, inc=1, device_id={"tp": t - 2}, device_id_type=MESH)

    @pl.when(z + 1 < chips)
    def _():
        pl.semaphore_signal(barrier, inc=1, device_id={"tp": t + 2}, device_id_type=MESH)

    pl.semaphore_signal(barrier, inc=1, device_id={"tp": t + 1 - 2 * c}, device_id_type=MESH)
    inner = (z > 0) & (z + 1 < chips)
    pl.semaphore_wait(barrier, jnp.where(inner, 3, 2) if chips > 1 else 1)

    load.wait()

    def pair_copy(b):
        return remote(
            pair_send.at[b], pair_recv.at[b], ps_sem.at[b], pr_sem.at[b], tp=t + 1 - 2 * c
        )

    def right_copy(b):
        return remote(stage.at[b], from_left.at[b], st_sem.at[b], left_sem.at[b], tp=t + 2)

    def left_copy(b):
        return remote(stage.at[b], from_right.at[b], st_sem.at[b], right_sem.at[b], tp=t - 2)

    def compute(b):
        other = aligned((2 * b + 1 - c) * rows, rows, ROWS)
        mine = aligned((2 * b + c) * rows, rows, ROWS)
        both = jnp.concatenate(
            [
                jnp.concatenate([attended[g, part, :] for g in range(attended.shape[0])], axis=1)
                for part in (other, mine)
            ],
            axis=0,
        )
        for n in range(width // chunk):
            cols = slice(n * chunk, (n + 1) * chunk)
            found = jnp.dot(both, weight[:, cols], preferred_element_type=jnp.float32)
            pair_send[b, :, cols] = found[:rows].astype(jnp.bfloat16)
            own[b, :, cols] = found[rows:]
        pair_copy(b).start()

    def combine(b):
        pair_copy(b).wait_recv()

        @pl.when(b > z)
        def _():
            @pl.when(z > 0)
            def _():
                right_copy(b).wait_recv()
                stage[b] = (
                    own[b] + pair_recv[b].astype(jnp.float32) + from_left[b].astype(jnp.float32)
                ).astype(jnp.bfloat16)

            @pl.when(z == 0)
            def _():
                stage[b] = (own[b] + pair_recv[b].astype(jnp.float32)).astype(jnp.bfloat16)

            right_copy(b).start()

        @pl.when(b < z)
        def _():
            @pl.when(z + 1 < chips)
            def _():
                left_copy(b).wait_recv()
                stage[b] = (
                    own[b] + pair_recv[b].astype(jnp.float32) + from_right[b].astype(jnp.float32)
                ).astype(jnp.bfloat16)

            @pl.when(z + 1 == chips)
            def _():
                stage[b] = (own[b] + pair_recv[b].astype(jnp.float32)).astype(jnp.bfloat16)

            left_copy(b).start()

    def place_of(j):
        d = chips - 1 - lax.div(j, 2)
        side = lax.rem(j, 2)
        b = z - d + 2 * d * side
        return b, (b >= 0) & (b < chips) & (d + 1 > side)

    at_end = (z == 0) | (z + 1 == chips)

    def first_pass(j, carry):
        b, valid = place_of(j)

        @pl.when(valid)
        def _():
            compute(b)

            @pl.when(at_end & (b != z))
            def _():
                combine(b)

        return carry

    lax.fori_loop(0, 2 * chips, first_pass, 0)

    def second_pass(j, carry):
        b, valid = place_of(j)

        @pl.when(valid & jnp.logical_not(at_end) & (b != z))
        def _():
            combine(b)

        return carry

    lax.fori_loop(0, 2 * chips, second_pass, 0)

    pair_copy(z).wait_recv()
    own[z] = own[z] + pair_recv[z].astype(jnp.float32)

    @pl.when(z > 0)
    def _():
        right_copy(z).wait_recv()
        own[z] = own[z] + from_left[z].astype(jnp.float32)

    @pl.when(z + 1 < chips)
    def _():
        left_copy(z).wait_recv()
        own[z] = own[z] + from_right[z].astype(jnp.float32)

    result[...] = (latent[...].astype(jnp.float32) + gate[...] * own[z]).astype(jnp.bfloat16)

    for b in range(chips):
        pair_copy(b).wait_send()

        @pl.when(b > z)
        def _():
            right_copy(b).wait_send()

        @pl.when(b < z)
        def _():
            left_copy(b).wait_send()


def tables(places, half):
    quarter = half // 4
    inverse = ROPE_BASE ** (-jnp.arange(quarter, dtype=jnp.float32) / quarter)
    by_row = (places // GRID_W).astype(jnp.float32)[:, None] * inverse
    by_col = (places % GRID_W).astype(jnp.float32)[:, None] * inverse
    angles = jnp.concatenate([by_row, by_row, by_col, by_col], axis=1)
    sign = jnp.where(jnp.arange(half) % (2 * quarter) < quarter, -1.0, 1.0)
    return jnp.cos(angles), jnp.sin(angles) * sign


def shards(
    sp_size,
    tp_size,
    latent,
    context,
    condition,
    context_condition,
    modulation,
    query_weight,
    key_weight,
    value_weight,
    lambdas,
    context_lift,
    head_gain,
    output_weight,
):
    rows, width = latent.shape
    chips = tp_size // 2
    local = query_weight.shape[1]
    heads = lambdas.shape[0]
    head = local // heads
    half = head // 2
    block_tokens = rows * tp_size
    ctx_rows = context.shape[0]
    piece = modulation.shape[2]
    places = lax.axis_index("sp") * block_tokens + jnp.arange(block_tokens, dtype=jnp.int32)
    cosine, sine = tables(places, half)
    vmem = pl.BlockSpec(memory_space=pltpu.VMEM)
    smem = pl.BlockSpec(memory_space=pltpu.SMEM)
    anywhere = pl.BlockSpec(memory_space=pl.ANY)
    bf16, f32 = jnp.bfloat16, jnp.float32
    dma = pltpu.SemaphoreType.DMA
    attended, gate = pl.pallas_call(
        functools.partial(attend_kernel, sp_size, tp_size),
        out_shape=(
            jax.ShapeDtypeStruct((heads, block_tokens, head), bf16),
            jax.ShapeDtypeStruct((1, width), f32),
        ),
        in_specs=[anywhere] * 2 + [vmem] * 2 + [anywhere] * 4 + [vmem] * 2 + [smem] * 2 + [vmem],
        out_specs=(vmem, vmem),
        scratch_shapes=[
            pltpu.VMEM((block_tokens, width), bf16),
            pltpu.VMEM(context.shape, bf16),
            pltpu.VMEM((max(2 * rows, ctx_rows), width), bf16),
            pltpu.VMEM(modulation.shape, bf16),
            pltpu.VMEM((width, local), bf16),
            pltpu.VMEM((width, local), bf16),
            pltpu.VMEM((width, local), bf16),
            pltpu.VMEM((sp_size * (ctx_rows + block_tokens), 2 * head), bf16),
            pltpu.VMEM((heads, block_tokens, head), bf16),
            pltpu.VMEM((heads, block_tokens + ctx_rows, 2 * head), bf16),
            pltpu.VMEM((heads, block_tokens, head), bf16),
            pltpu.VMEM((heads, block_tokens, head), bf16),
            pltpu.VMEM((sp_size, 8, piece), f32),
            pltpu.VMEM((tp_size, 8, piece), f32),
            pltpu.VMEM((8, width), f32),
            dma((6,)),
            dma((3, chips)),
            dma((tp_size,)),
            dma((sp_size,)),
            dma((sp_size,)),
            dma((tp_size,)),
            dma((tp_size,)),
            dma((sp_size, chips + 1)),
            dma((sp_size, chips + 1)),
            dma((heads, chips)),
            dma((heads, chips)),
            dma((heads,)),
            dma((heads,)),
        ],
        compiler_params=pltpu.CompilerParams(
            collective_id=0, has_side_effects=True, vmem_limit_bytes=VMEM_LIMIT
        ),
        name="attend",
    )(
        latent,
        context,
        condition.reshape(1, -1),
        context_condition.reshape(1, -1),
        modulation,
        query_weight,
        key_weight,
        value_weight,
        cosine,
        sine,
        lambdas,
        context_lift,
        head_gain.reshape(1, -1),
    )
    blocks = (chips, rows, width)
    return pl.pallas_call(
        functools.partial(output_kernel, tp_size),
        out_shape=jax.ShapeDtypeStruct((rows, width), bf16),
        in_specs=[vmem, anywhere, vmem, vmem],
        out_specs=vmem,
        scratch_shapes=[
            pltpu.VMEM(output_weight.shape, bf16),
            pltpu.VMEM(blocks, f32),
            pltpu.VMEM(blocks, bf16),
            pltpu.VMEM(blocks, bf16),
            pltpu.VMEM(blocks, bf16),
            pltpu.VMEM(blocks, bf16),
            pltpu.VMEM(blocks, bf16),
            dma(()),
            dma((chips,)),
            dma((chips,)),
            dma((chips,)),
            dma((chips,)),
            dma((chips,)),
        ],
        compiler_params=pltpu.CompilerParams(
            collective_id=1, has_side_effects=True, vmem_limit_bytes=VMEM_LIMIT
        ),
        name="output",
    )(attended, output_weight, latent, gate)


def solution(mesh):
    in_specs = (
        P(("sp", "tp"), None),
        P("sp", None),
        P(),
        P(),
        P(None, "sp", "tp"),
        P(None, "tp"),
        P(None, "tp"),
        P(None, "tp"),
        P("tp"),
        P("tp"),
        P(),
        P("tp", None),
    )
    out_specs = P(("sp", "tp"), None)
    body = functools.partial(shards, mesh.shape["sp"], mesh.shape["tp"])
    return jax.shard_map(body, mesh=mesh, in_specs=in_specs, out_specs=out_specs, check_vma=False)
```

```python
import functools

import jax
import jax.numpy as jnp
from jax import lax
from jax.experimental import pallas as pl
from jax.experimental.pallas import tpu as pltpu
from jax.sharding import PartitionSpec as P

GRID_W = 64
ROPE_BASE = 10000.0
EPSILON = 1e-05
LOG2E = 1.4426950408889634
ROWS = 16
VMEM_LIMIT = 62 * 1024 * 1024
MESH = pl.DeviceIdType.MESH


def remote(src, dst, send_sem, recv_sem, **where):
    return pltpu.make_async_remote_copy(
        src_ref=src,
        dst_ref=dst,
        send_sem=send_sem,
        recv_sem=recv_sem,
        device_id=where,
        device_id_type=MESH,
    )


def aligned(start, size, unit):
    return pl.ds(pl.multiple_of(start, unit), size)


def attend_kernel(
    sp_size,
    tp_size,
    latent,
    context,
    condition,
    context_condition,
    modulation,
    query_weight,
    key_weight,
    value_weight,
    cosine,
    sine,
    lambdas,
    lift,
    gain,
    attended,
    gate,
    tokens,
    context_tokens,
    normed,
    mod_weight,
    wq,
    wk,
    wv,
    keys_values,
    queries,
    kv_stage,
    q_stage,
    out_stage,
    mod_parts,
    mod_pieces,
    mod_rows,
    local_sem,
    tok_send,
    tok_recv,
    part_send,
    part_recv,
    piece_send,
    piece_recv,
    kv_send,
    kv_recv,
    q_send,
    q_recv,
    out_send,
    out_recv,
):
    s = lax.axis_index("sp")
    t = lax.axis_index("tp")
    z = lax.div(t, 2)
    c = lax.rem(t, 2)
    chips = tp_size // 2
    rows, width = latent.shape
    pair = 2 * rows
    block_tokens = tp_size * rows
    ctx_rows = context.shape[0]
    ctx_total = ctx_rows * sp_size
    local = query_weight.shape[1]
    heads = lambdas.shape[0]
    head = local // heads
    half = head // 2
    piece = modulation.shape[2]
    depth = modulation.shape[1]

    own_slot = tokens.at[aligned(t * rows, rows, ROWS)]
    locals_ = [
        pltpu.make_async_copy(src, dst, local_sem.at[i])
        for i, (src, dst) in enumerate(
            [
                (modulation, mod_weight),
                (latent, own_slot),
                (context, context_tokens),
                (key_weight, wk),
                (value_weight, wv),
                (query_weight, wq),
            ]
        )
    ]
    for copy in locals_:
        copy.start()

    barrier = pltpu.get_barrier_semaphore()
    for k in range(1, tp_size):
        pl.semaphore_signal(
            barrier, inc=1, device_id={"tp": lax.rem(t + k, tp_size)}, device_id_type=MESH
        )
    for k in range(1, sp_size):
        pl.semaphore_signal(
            barrier, inc=1, device_id={"sp": lax.rem(s + k, sp_size)}, device_id_type=MESH
        )
    pl.semaphore_wait(barrier, tp_size + sp_size - 2)

    part_rows = rows // 2

    def token_copy(kind, b, core, part, own=False):
        slot = 2 * b + core
        place = tokens.at[aligned(slot * rows + part * part_rows, part_rows, ROWS)]
        to = (t + 2, t - 2, t + 1 - 2 * c)[kind]
        return remote(
            latent.at[part * part_rows : (part + 1) * part_rows] if own else place,
            place,
            tok_send.at[kind, 2 * b + part],
            tok_recv.at[2 * slot + part],
            tp=to,
        )

    for part in range(2):

        @pl.when(z + 1 < chips)
        def _():
            token_copy(0, z, c, part, True).start()

        @pl.when(z > 0)
        def _():
            token_copy(1, z, c, part, True).start()

        token_copy(2, z, c, part, True).start()

    def silu(ref):
        v = ref[:, aligned(s * depth, depth, 128)]
        return v / (1.0 + jnp.exp(-v))

    first = silu(condition)
    second = silu(context_condition)
    which = lax.broadcasted_iota(jnp.int32, (ROWS, depth), 0)
    vectors = jnp.where(
        which == 0, jnp.broadcast_to(first, (ROWS, depth)), jnp.broadcast_to(second, (ROWS, depth))
    ).astype(jnp.bfloat16)
    locals_[0].wait()
    for r in range(3):
        found = jnp.dot(vectors, mod_weight[r], preferred_element_type=jnp.float32)
        mod_parts[s, 2 * r : 2 * r + 2, :] = found[0:2]
    mod_parts[s, 6:8, :] = jnp.zeros((2, piece), jnp.float32)

    def part_copy(k, owner):
        return remote(
            mod_parts.at[owner],
            mod_parts.at[owner],
            part_send.at[k],
            part_recv.at[owner],
            sp=lax.rem(s + k, sp_size),
        )

    def piece_copy(k, owner):
        return remote(
            mod_pieces.at[owner],
            mod_pieces.at[owner],
            piece_send.at[k],
            piece_recv.at[owner],
            tp=lax.rem(t + k, tp_size),
        )

    for k in range(1, sp_size):
        part_copy(k, s).start()
    for k in range(1, sp_size):
        part_copy(k, lax.rem(s + k, sp_size)).wait_recv()
    total = mod_parts[0]
    for i in range(1, sp_size):
        total = total + mod_parts[i]
    mod_pieces[t] = total
    for k in range(1, tp_size):
        piece_copy(k, t).start()

    def forward(d):
        left = z - d
        right = z + d

        for part in range(2):

            @pl.when(left >= 0)
            def _():
                token_copy(2, left, c, part).wait_recv()

                @pl.when(z + 1 < chips)
                def _():
                    token_copy(0, left, c, part).start()

                token_copy(2, left, c, part).start()

            @pl.when(right < chips)
            def _():
                token_copy(2, right, c, part).wait_recv()

                @pl.when(z > 0)
                def _():
                    token_copy(1, right, c, part).start()

                token_copy(2, right, c, part).start()

    forward(1)
    for k in range(1, tp_size):
        piece_copy(k, lax.rem(t + k, tp_size)).wait_recv()
    for i in range(tp_size):
        mod_rows[:, i * piece : (i + 1) * piece] = mod_pieces[i]
    gate[...] = mod_rows[4:5, :]

    def normalise(source, base, count, row):
        def group(i, carry):
            x = source[aligned(base + i * ROWS, ROWS, ROWS), :].astype(jnp.float32)
            x = x - jnp.sum(x, axis=1, keepdims=True) * (1.0 / width)
            spread = jnp.sum(x * x, axis=1, keepdims=True) * (1.0 / width)
            y = x * lax.rsqrt(spread + EPSILON)
            y = y * (1.0 + mod_rows[2 + row : 3 + row, :]) + mod_rows[row : row + 1, :]
            normed[aligned(i * ROWS, ROWS, ROWS), :] = y.astype(jnp.bfloat16)
            return carry

        lax.fori_loop(0, count // ROWS, group, 0)

    my_head = lax.rem(s, heads)

    def mate(k):
        return lax.rem(my_head + k, heads)

    def kv_place(owner, b, is_context):
        if is_context:
            return aligned(owner * ctx_rows, ctx_rows, ROWS)
        return aligned(ctx_total + owner * block_tokens + b * pair, pair, ROWS)

    def stage_place(b, is_context):
        if is_context:
            return aligned(block_tokens, ctx_rows, ROWS)
        return aligned(b * pair, pair, ROWS)

    def kv_copy(k, owner, b, is_context):
        to = lax.rem(s + k, sp_size)
        return remote(
            kv_stage.at[lax.rem(to, heads), stage_place(b, is_context)],
            keys_values.at[kv_place(owner, b, is_context)],
            kv_send.at[k, b],
            kv_recv.at[owner, b],
            sp=to,
        )

    def q_copy(k, slot, b):
        place = aligned(b * pair, pair, ROWS)
        return remote(
            q_stage.at[mate(k), place],
            queries.at[slot, place],
            q_send.at[k, b],
            q_recv.at[slot, b],
            sp=s - my_head + mate(k),
        )

    def out_copy(k, head_index):
        return remote(
            out_stage.at[mate(k)],
            attended.at[head_index],
            out_send.at[k],
            out_recv.at[head_index],
            sp=s - my_head + mate(k),
        )

    def hand_out(keys, values, b, is_context):
        place = stage_place(b, is_context)
        for g in range(heads):
            kv_stage[g, place, :head] = keys[:, g * head : (g + 1) * head]
            kv_stage[g, place, head:] = values[:, g * head : (g + 1) * head]
        for k in range(1, sp_size):
            kv_copy(k, s, b, is_context).start()
        keys_values[kv_place(s, b, is_context), :] = kv_stage[my_head, place, :]

    locals_[1].wait()
    for i in (3, 4, 5):
        locals_[i].wait()

    quarter = half // 4
    lane = lax.broadcasted_iota(jnp.int32, (pair, half), 1)
    low = lax.rem(lane, 2 * quarter) < quarter

    def turn(raw, b):
        cos = cosine[aligned(b * pair, pair, ROWS), :]
        sin = sine[aligned(b * pair, pair, ROWS), :]
        parts = []
        for i in range(local // half):
            v = raw[:, i * half : (i + 1) * half].astype(jnp.bfloat16).astype(jnp.float32)
            other = jnp.where(low, pltpu.roll(v, half - quarter, 1), pltpu.roll(v, quarter, 1))
            parts.append((v * cos + other * sin).astype(jnp.bfloat16))
        return jnp.concatenate(parts, axis=1)

    def process(b):
        for part in range(2):
            token_copy(2, b, 1 - c, part).wait_recv()
        normalise(tokens, b * pair, pair, 0)
        x = normed[:pair, :]
        hand_out(
            turn(jnp.dot(x, wk[...], preferred_element_type=jnp.float32), b),
            jnp.dot(x, wv[...], preferred_element_type=jnp.float32).astype(jnp.bfloat16),
            b,
            False,
        )
        turned = turn(jnp.dot(x, wq[...], preferred_element_type=jnp.float32), b)
        place = aligned(b * pair, pair, ROWS)
        for g in range(heads):
            q_stage[g, place, :] = turned[:, g * head : (g + 1) * head]
        for k in range(1, heads):
            q_copy(k, my_head, b).start()
        queries[my_head, place, :] = q_stage[my_head, place, :]

    def process_context():
        locals_[2].wait()
        normalise(context_tokens, 0, ctx_rows, 1)
        hand_out(
            jnp.dot(normed[:ctx_rows, :], wk[...], preferred_element_type=jnp.float32).astype(
                jnp.bfloat16
            ),
            jnp.dot(normed[:ctx_rows, :], wv[...], preferred_element_type=jnp.float32).astype(
                jnp.bfloat16
            ),
            chips,
            True,
        )

    def step(j, carry):
        d = lax.div(j, 2)
        side = lax.rem(j, 2)

        @pl.when(j == 1)
        def _():
            if chips > 2:
                forward(2)
            process_context()

        @pl.when((side == 0) & (d >= 2) & (d + 1 < chips))
        def _():
            forward(d + 1)

        b = z - d + 2 * d * side

        @pl.when((b >= 0) & (b < chips) & (d + 1 > side))
        def _():
            process(b)

        return carry

    lax.fori_loop(0, 2 * chips, step, 0)

    for k in range(1, sp_size):
        owner = lax.rem(s + k, sp_size)
        kv_copy(k, owner, chips, True).wait_recv()
        for b in range(chips):
            kv_copy(k, owner, b, False).wait_recv()
    for k in range(1, heads):
        for b in range(chips):
            q_copy(k, mate(k), b).wait_recv()

    tile = min(256, block_tokens)
    key_total = keys_values.shape[0]
    factor = half ** (-0.5) * LOG2E
    on_context = lax.broadcasted_iota(jnp.int32, (1, key_total), 1) < ctx_total

    raised = jnp.where(on_context, lift[my_head] * LOG2E, 0.0)
    weight_of_second = lambdas[my_head]

    def attention(i, slot):
        place = aligned(i * tile, tile, ROWS)
        outs = []
        for m in range(2):
            scores = lax.dot_general(
                queries[slot, place, m * half : (m + 1) * half],
                keys_values[:, m * half : (m + 1) * half],
                (((1,), (1,)), ((), ())),
                preferred_element_type=jnp.float32,
            )
            scores = scores * factor + raised
            weights = jnp.exp2(scores - jnp.max(scores, axis=1, keepdims=True))
            sums = jnp.sum(weights, axis=1, keepdims=True)
            outs.append(
                jnp.dot(
                    weights.astype(jnp.bfloat16),
                    keys_values[:, head:],
                    preferred_element_type=jnp.float32,
                )
                / sums
            )
        diff = outs[0] - weight_of_second * outs[1]
        mean = jnp.sum(diff * diff, axis=1, keepdims=True) * (1.0 / head)
        out_stage[slot, place, :] = (diff * lax.rsqrt(mean + EPSILON) * gain[...]).astype(
            jnp.bfloat16
        )
        return slot

    for k in range(1, heads + 1):
        lax.fori_loop(0, block_tokens // tile, attention, mate(k))
        if k < heads:
            out_copy(k, my_head).start()
    attended[my_head] = out_stage[my_head]
    for k in range(1, heads):
        out_copy(k, mate(k)).wait_recv()
        out_copy(k, my_head).wait_send()
        for b in range(chips):
            q_copy(k, my_head, b).wait_send()

    for b in range(chips):
        for part in range(2):

            @pl.when((b <= z) & (z + 1 < chips))
            def _():
                token_copy(0, b, c, part).wait_send()

            @pl.when((b >= z) & (z > 0))
            def _():
                token_copy(1, b, c, part).wait_send()

            token_copy(2, b, c, part).wait_send()
    for k in range(1, tp_size):
        piece_copy(k, t).wait_send()
    for k in range(1, sp_size):
        part_copy(k, s).wait_send()
        kv_copy(k, s, chips, True).wait_send()
        for b in range(chips):
            kv_copy(k, s, b, False).wait_send()


def output_kernel(
    tp_size,
    attended,
    output_weight,
    latent,
    gate,
    result,
    weight,
    own,
    pair_send,
    pair_recv,
    stage,
    from_left,
    from_right,
    local_sem,
    ps_sem,
    pr_sem,
    st_sem,
    left_sem,
    right_sem,
):
    t = lax.axis_index("tp")
    z = lax.div(t, 2)
    c = lax.rem(t, 2)
    chips = tp_size // 2
    rows, width = latent.shape
    span = width // 2
    chunk = min(1024, span)

    load = pltpu.make_async_copy(output_weight, weight, local_sem)
    load.start()
    barrier = pltpu.get_barrier_semaphore()

    @pl.when(z > 0)
    def _():
        pl.semaphore_signal(barrier, inc=1, device_id={"tp": t - 2}, device_id_type=MESH)

    @pl.when(z + 1 < chips)
    def _():
        pl.semaphore_signal(barrier, inc=1, device_id={"tp": t + 2}, device_id_type=MESH)

    pl.semaphore_signal(barrier, inc=1, device_id={"tp": t + 1 - 2 * c}, device_id_type=MESH)
    inner = (z > 0) & (z + 1 < chips)
    pl.semaphore_wait(barrier, jnp.where(inner, 3, 2) if chips > 1 else 1)

    load.wait()

    def pair_copy(b):
        return remote(
            pair_send.at[b], pair_recv.at[b], ps_sem.at[b], pr_sem.at[b], tp=t + 1 - 2 * c
        )

    def right_copy(b):
        return remote(stage.at[b], from_left.at[b], st_sem.at[b], left_sem.at[b], tp=t + 2)

    def left_copy(b):
        return remote(stage.at[b], from_right.at[b], st_sem.at[b], right_sem.at[b], tp=t - 2)

    def compute(b, part):
        u = 2 * b + part
        other = aligned((2 * b + 1 - c) * rows, rows, ROWS)
        mine = aligned((2 * b + c) * rows, rows, ROWS)
        both = jnp.concatenate(
            [
                jnp.concatenate([attended[g, part, :] for g in range(attended.shape[0])], axis=1)
                for part in (other, mine)
            ],
            axis=0,
        )
        for n in range(span // chunk):
            cols = slice(n * chunk, (n + 1) * chunk)
            found = jnp.dot(
                both,
                weight[:, aligned(part * span + n * chunk, chunk, 128)],
                preferred_element_type=jnp.float32,
            )
            pair_send[u, :, cols] = found[:rows].astype(jnp.bfloat16)
            own[u, :, cols] = found[rows:]
        pair_copy(u).start()

    def combine(b, part):
        u = 2 * b + part
        pair_copy(u).wait_recv()

        @pl.when(b > z)
        def _():
            @pl.when(z > 0)
            def _():
                right_copy(u).wait_recv()
                stage[u] = (
                    own[u] + pair_recv[u].astype(jnp.float32) + from_left[u].astype(jnp.float32)
                ).astype(jnp.bfloat16)

            @pl.when(z == 0)
            def _():
                stage[u] = (own[u] + pair_recv[u].astype(jnp.float32)).astype(jnp.bfloat16)

            right_copy(u).start()

        @pl.when(b < z)
        def _():
            @pl.when(z + 1 < chips)
            def _():
                left_copy(u).wait_recv()
                stage[u] = (
                    own[u] + pair_recv[u].astype(jnp.float32) + from_right[u].astype(jnp.float32)
                ).astype(jnp.bfloat16)

            @pl.when(z + 1 == chips)
            def _():
                stage[u] = (own[u] + pair_recv[u].astype(jnp.float32)).astype(jnp.bfloat16)

            left_copy(u).start()

    def place_of(j):
        d = chips - 1 - lax.div(j, 4)
        side = lax.rem(lax.div(j, 2), 2)
        b = z - d + 2 * d * side
        return b, lax.rem(j, 2), (b >= 0) & (b < chips) & (d + 1 > side)

    at_end = (z == 0) | (z + 1 == chips)

    def first_pass(j, carry):
        b, part, valid = place_of(j)

        @pl.when(valid)
        def _():
            compute(b, part)

            @pl.when(at_end & (b != z))
            def _():
                combine(b, part)

        return carry

    lax.fori_loop(0, 4 * chips, first_pass, 0)

    def second_pass(j, carry):
        b, part, valid = place_of(j)

        @pl.when(valid & jnp.logical_not(at_end) & (b != z))
        def _():
            combine(b, part)

        return carry

    lax.fori_loop(0, 4 * chips, second_pass, 0)

    for part in range(2):
        u = 2 * z + part
        cols = slice(part * span, (part + 1) * span)
        pair_copy(u).wait_recv()
        own[u] = own[u] + pair_recv[u].astype(jnp.float32)

        @pl.when(z > 0)
        def _():
            right_copy(u).wait_recv()
            own[u] = own[u] + from_left[u].astype(jnp.float32)

        @pl.when(z + 1 < chips)
        def _():
            left_copy(u).wait_recv()
            own[u] = own[u] + from_right[u].astype(jnp.float32)

        result[:, cols] = (latent[:, cols].astype(jnp.float32) + gate[:, cols] * own[u]).astype(
            jnp.bfloat16
        )

    for u in range(2 * chips):
        pair_copy(u).wait_send()

        @pl.when(u // 2 > z)
        def _():
            right_copy(u).wait_send()

        @pl.when(u // 2 < z)
        def _():
            left_copy(u).wait_send()


def tables(places, half):
    quarter = half // 4
    inverse = ROPE_BASE ** (-jnp.arange(quarter, dtype=jnp.float32) / quarter)
    by_row = (places // GRID_W).astype(jnp.float32)[:, None] * inverse
    by_col = (places % GRID_W).astype(jnp.float32)[:, None] * inverse
    angles = jnp.concatenate([by_row, by_row, by_col, by_col], axis=1)
    sign = jnp.where(jnp.arange(half) % (2 * quarter) < quarter, -1.0, 1.0)
    return jnp.cos(angles), jnp.sin(angles) * sign


def shards(
    sp_size,
    tp_size,
    latent,
    context,
    condition,
    context_condition,
    modulation,
    query_weight,
    key_weight,
    value_weight,
    lambdas,
    context_lift,
    head_gain,
    output_weight,
):
    rows, width = latent.shape
    chips = tp_size // 2
    local = query_weight.shape[1]
    heads = lambdas.shape[0]
    head = local // heads
    half = head // 2
    block_tokens = rows * tp_size
    ctx_rows = context.shape[0]
    piece = modulation.shape[2]
    places = lax.axis_index("sp") * block_tokens + jnp.arange(block_tokens, dtype=jnp.int32)
    cosine, sine = tables(places, half)
    vmem = pl.BlockSpec(memory_space=pltpu.VMEM)
    smem = pl.BlockSpec(memory_space=pltpu.SMEM)
    anywhere = pl.BlockSpec(memory_space=pl.ANY)
    bf16, f32 = jnp.bfloat16, jnp.float32
    dma = pltpu.SemaphoreType.DMA
    attended, gate = pl.pallas_call(
        functools.partial(attend_kernel, sp_size, tp_size),
        out_shape=(
            jax.ShapeDtypeStruct((heads, block_tokens, head), bf16),
            jax.ShapeDtypeStruct((1, width), f32),
        ),
        in_specs=[anywhere] * 2 + [vmem] * 2 + [anywhere] * 4 + [vmem] * 2 + [smem] * 2 + [vmem],
        out_specs=(vmem, vmem),
        scratch_shapes=[
            pltpu.VMEM((block_tokens, width), bf16),
            pltpu.VMEM(context.shape, bf16),
            pltpu.VMEM((max(2 * rows, ctx_rows), width), bf16),
            pltpu.VMEM(modulation.shape, bf16),
            pltpu.VMEM((width, local), bf16),
            pltpu.VMEM((width, local), bf16),
            pltpu.VMEM((width, local), bf16),
            pltpu.VMEM((sp_size * (ctx_rows + block_tokens), 2 * head), bf16),
            pltpu.VMEM((heads, block_tokens, head), bf16),
            pltpu.VMEM((heads, block_tokens + ctx_rows, 2 * head), bf16),
            pltpu.VMEM((heads, block_tokens, head), bf16),
            pltpu.VMEM((heads, block_tokens, head), bf16),
            pltpu.VMEM((sp_size, 8, piece), f32),
            pltpu.VMEM((tp_size, 8, piece), f32),
            pltpu.VMEM((8, width), f32),
            dma((6,)),
            dma((3, 2 * chips)),
            dma((2 * tp_size,)),
            dma((sp_size,)),
            dma((sp_size,)),
            dma((tp_size,)),
            dma((tp_size,)),
            dma((sp_size, chips + 1)),
            dma((sp_size, chips + 1)),
            dma((heads, chips)),
            dma((heads, chips)),
            dma((heads,)),
            dma((heads,)),
        ],
        compiler_params=pltpu.CompilerParams(
            collective_id=0, has_side_effects=True, vmem_limit_bytes=VMEM_LIMIT
        ),
        name="attend",
    )(
        latent,
        context,
        condition.reshape(1, -1),
        context_condition.reshape(1, -1),
        modulation,
        query_weight,
        key_weight,
        value_weight,
        cosine,
        sine,
        lambdas,
        context_lift,
        head_gain.reshape(1, -1),
    )
    blocks = (2 * chips, rows, width // 2)
    return pl.pallas_call(
        functools.partial(output_kernel, tp_size),
        out_shape=jax.ShapeDtypeStruct((rows, width), bf16),
        in_specs=[vmem, anywhere, vmem, vmem],
        out_specs=vmem,
        scratch_shapes=[
            pltpu.VMEM(output_weight.shape, bf16),
            pltpu.VMEM(blocks, f32),
            pltpu.VMEM(blocks, bf16),
            pltpu.VMEM(blocks, bf16),
            pltpu.VMEM(blocks, bf16),
            pltpu.VMEM(blocks, bf16),
            pltpu.VMEM(blocks, bf16),
            dma(()),
            dma((2 * chips,)),
            dma((2 * chips,)),
            dma((2 * chips,)),
            dma((2 * chips,)),
            dma((2 * chips,)),
        ],
        compiler_params=pltpu.CompilerParams(
            collective_id=1, has_side_effects=True, vmem_limit_bytes=VMEM_LIMIT
        ),
        name="output",
    )(attended, output_weight, latent, gate)


def solution(mesh):
    in_specs = (
        P(("sp", "tp"), None),
        P("sp", None),
        P(),
        P(),
        P(None, "sp", "tp"),
        P(None, "tp"),
        P(None, "tp"),
        P(None, "tp"),
        P("tp"),
        P("tp"),
        P(),
        P("tp", None),
    )
    out_specs = P(("sp", "tp"), None)
    body = functools.partial(shards, mesh.shape["sp"], mesh.shape["tp"])
    return jax.shard_map(body, mesh=mesh, in_specs=in_specs, out_specs=out_specs, check_vma=False)
```
